128 devices in a mesh: ep: 128 (over z, y, x, core).
Axes of the slice: x: 4, y: 4, z: 4, core: 2. Of those that a mesh axis runs over, the one named last changes fastest.
Arguments:
- tokens: bfloat16 [8192, 2048], P('ep'), may hold values from -6 to 6
- conv_state: bfloat16 [8192, 3, 1024], P('ep'), may hold values from -6 to 6
- recur_state: float32 [8192, 1024], P('ep'), may hold values from -6 to 6
- w_branch: bfloat16 [2048, 1024], replicated, may hold values from -0.125 to 0.125
- w_gate: bfloat16 [2048, 1024], replicated, may hold values from -0.125 to 0.125
- conv_taps: float32 [4, 1024], replicated, may hold values from -3 to 3
- rate_blocks: bfloat16 [16, 64, 64], replicated, may hold values from -0.75 to 0.75
- input_blocks: bfloat16 [16, 64, 64], replicated, may hold values from -0.75 to 0.75
- decay_param: float32 [1024], replicated, may hold values from 1.5 to 6.5
- w_mix: bfloat16 [1024, 2048], replicated, may hold values from -0.1875 to 0.1875
- gain_pre: float32 [2048], replicated, may hold values from 0.1 to 1.9
- gain_post: float32 [2048], replicated, may hold values from 0.1 to 1.9
- gain_ffn: float32 [2048], replicated, may hold values from 0.1 to 1.9
- gain_out: float32 [2048], replicated, may hold values from 0.1 to 1.9
- routes: int32 [8192, 2], P('ep'), may hold values from 0 to 127, all different within a row; in each aligned block of 64 rows (0 to 63, 64 to 127, ...) at most 3 rows name the same one
- affinity: float32 [8192, 2], P('ep'), may hold values from 0.05 to 1
- w_expert_gate: bfloat16 [128, 2048, 512], P('ep'), may hold values from -0.125 to 0.125
- w_expert_up: bfloat16 [128, 2048, 512], P('ep'), may hold values from -0.125 to 0.125
- w_expert_down: bfloat16 [128, 512, 2048], P('ep'), may hold values from -0.25 to 0.25
Outputs:
- layer_out: bfloat16 [8192, 2048], P('ep')
- conv_next: bfloat16 [8192, 3, 1024], P('ep')
- state_next: float32 [8192, 1024], P('ep')
The draws below stay inside these ranges and needn't reach their ends.
Inputs may be any that keep to these rules, and one draw needn't show every extreme that they name: `routes`: each row names 2 different experts. Among the 64 rows of one device no expert is named more than 3 times, and in every draw some device names some expert exactly 3 times.
All inputs are finite; a program needn't handle non-finite values.
Results may differ from the reference program's by a relative error of at most 0.014.
Values may be sent and summed in bfloat16 or wider, within the bound.
A program may use at most 128 MiB of HBM per device.

```python
import math
import jax
import jax.numpy as jnp
import numpy as np
from jax import lax

D = 2048
BW = 1024
NB = 16
BS = 64
TAPS = 4
FF = 512
TOP_K = 2
SEQ_DEV = 64
TOKENS = 8192
EXPERTS = 128
CAP = 3
LIMIT = 64


def block_scale(own_key, extent, cuts, least, largest):
    def one(position, parts):
        heights = jax.random.uniform(jax.random.fold_in(jax.random.fold_in(own_key, 6), position), (parts,), jnp.float32, least / len(cuts), largest / len(cuts))
        return jnp.repeat(jnp.exp(heights), extent[position] // parts).reshape((-1,) + (1,) * (len(extent) - position - 1))

    factor_of = one(*cuts[0])
    for cut in cuts[1:]:
        factor_of = factor_of * one(*cut)
    return factor_of


def deal_out(key, own, number, rows, count, top, reach, slope):
    sequence = jax.random.permutation(key, count)
    packed, common = portions_of(count, rows * top, reach, slope, True), portions_of(count, rows * top, reach, slope, False)
    places = jnp.arange(count)

    def named(lengths, offset_by):
        used = int((lengths > 0).sum())
        fixed = max(1, used // 4)
        passed = fixed + (places - fixed + offset_by * (used - fixed)) % max(1, count - fixed)
        return jnp.zeros((count,), jnp.int32).at[sequence[jnp.where(places < fixed, places, passed)]].set(jnp.asarray(lengths, jnp.int32))

    lengths = jnp.where(number % 4 == 0, named(packed, number // 4), named(common, number - number // 4 - 1))
    mixed = jax.random.permutation(jax.random.fold_in(own, 3), count)
    donor, sink = mixed[0:count // 2 * 2:2], mixed[1:count // 2 * 2:2]
    margin = jnp.minimum(lengths[donor] - 1, reach - lengths[sink]) // 2
    margin = jnp.where((donor == sequence[0]) | (sink == sequence[0]) | (lengths[sink] == 0), 0, jnp.maximum(margin, 0))
    passed = jax.random.randint(jax.random.fold_in(own, 4), (count // 2,), 0, 1 << 20) % (margin + 1)
    lengths = lengths.at[donor].add(-passed).at[sink].add(passed)
    labels = jnp.searchsorted(jnp.cumsum(lengths), jnp.arange(rows * top), side="right").astype(jnp.int32)
    listing = labels.reshape(top, rows).T
    listing = listing[jax.random.permutation(jax.random.fold_in(own, 1), rows)]
    offset_by = jax.random.randint(jax.random.fold_in(own, 2), (rows, 1), 0, top)
    return jnp.take_along_axis(listing, (jnp.arange(top)[None, :] + offset_by) % top, axis=1)


def portions_of(count, total, reach, skew, full):
    portions = [(1 << 20) // math.isqrt(standing ** skew) + 1 for standing in range(1, count + 1)]
    largest = reach if full else min(reach, max(-(-total // count), total * portions[0] // sum(portions)))
    least = 1 if total - largest >= count - 1 else 0
    given, surplus = [largest] + [least] * (count - 1), total - largest - least * (count - 1)
    while surplus > 0:
        movable = [i for i in range(1, count) if given[i] < largest] or [i for i in range(1, count) if given[i] < reach]
        whole, left = sum([portions[i] for i in movable]), surplus
        for i in movable:
            more = min(reach - given[i], max(1, left * portions[i] // whole), surplus)
            given[i] = given[i] + more
            surplus = surplus - more
    return np.array(given)


def gaussian(own_key, dims, deviation, limit, shards=(), kind=jnp.bfloat16):
    values = jax.random.normal(own_key, dims, jnp.float32) * deviation
    if len(shards) > 0:
        values = block_scale(own_key, dims, shards, -0.22, 0.18) * values
    return jnp.clip(values, min=-limit, max=limit).astype(kind)


def setup_inputs(seed: int = 0) -> dict:
    streams_of = jax.random.split(jax.random.key(seed), 20)
    tokens = gaussian(streams_of[0], (TOKENS, D), 1.0, 6.0, ((0, 128),))
    conv_state = gaussian(streams_of[1], (TOKENS, TAPS - 1, BW), 1.0, 6.0, ((0, 128),))
    recur_state = gaussian(streams_of[2], (TOKENS, BW), 1.0, 6.0, ((0, 128),), jnp.float32)
    w_branch = gaussian(streams_of[3], (D, BW), D ** -0.5, 0.125)
    w_gate = gaussian(streams_of[4], (D, BW), D ** -0.5, 0.125)
    conv_taps = gaussian(streams_of[5], (TAPS, BW), TAPS ** -0.5, 3.0, (), jnp.float32)
    rate_blocks = gaussian(streams_of[6], (NB, BS, BS), BS ** -0.5, 0.75)
    input_blocks = gaussian(streams_of[7], (NB, BS, BS), BS ** -0.5, 0.75)
    decay_param = jnp.clip(jax.random.uniform(streams_of[8], (BW,), jnp.float32, 1.5, 6.5), 1.5, 6.5)
    w_mix = gaussian(streams_of[9], (BW, D), BW ** -0.5, 0.1875)
    gain_pre = jnp.clip(1.0 + 0.18 * jax.random.normal(streams_of[10], (D,), jnp.float32), 0.1, 1.9)
    gain_post = jnp.clip(1.0 + 0.18 * jax.random.normal(streams_of[11], (D,), jnp.float32), 0.1, 1.9)
    gain_ffn = jnp.clip(1.0 + 0.18 * jax.random.normal(streams_of[12], (D,), jnp.float32), 0.1, 1.9)
    gain_out = jnp.clip(1.0 + 0.18 * jax.random.normal(streams_of[13], (D,), jnp.float32), 0.1, 1.9)
    routes_keys = jax.random.split(jax.random.fold_in(streams_of[14], 1), TOKENS // SEQ_DEV)
    routes_turns = jax.random.permutation(jax.random.fold_in(streams_of[14], 3), TOKENS // SEQ_DEV)
    routes = jax.vmap(lambda own, number: deal_out(jax.random.fold_in(streams_of[14], 2), own, number, SEQ_DEV, EXPERTS, TOP_K, CAP, 2))(routes_keys, routes_turns).reshape((TOKENS, TOP_K))
    affinity = jnp.clip(jnp.exp(math.log(1.0) - 2.9957323 * jax.random.uniform(streams_of[15], (TOKENS, TOP_K), jnp.float32) ** block_scale(streams_of[15], (TOKENS, TOP_K), ((0, 128),), -0.2, 0.2)), 0.05, 1.0)
    w_expert_gate = gaussian(streams_of[16], (EXPERTS, D, FF), D ** -0.5, 0.125, ((0, 128),))
    w_expert_up = gaussian(streams_of[17], (EXPERTS, D, FF), D ** -0.5, 0.125, ((0, 128),))
    w_expert_down = gaussian(streams_of[18], (EXPERTS, FF, D), FF ** -0.5, 0.25, ((0, 128),))
    return dict(tokens=tokens, conv_state=conv_state, recur_state=recur_state, w_branch=w_branch, w_gate=w_gate, conv_taps=conv_taps, rate_blocks=rate_blocks, input_blocks=input_blocks, decay_param=decay_param, w_mix=w_mix, gain_pre=gain_pre, gain_post=gain_post, gain_ffn=gain_ffn, gain_out=gain_out, routes=routes, affinity=affinity, w_expert_gate=w_expert_gate, w_expert_up=w_expert_up, w_expert_down=w_expert_down)


epsilon = 1e-06
gate_scale = 8.0

def norm_rows(values, gain_vec):
    floats = values.astype(jnp.float32)
    inv_scale = lax.rsqrt(lax.optimization_barrier(jnp.mean(floats * floats, axis=-1, keepdims=True)) + epsilon)
    return floats * inv_scale * gain_vec.astype(jnp.float32)

def recurrence(tokens, conv_state, recur_state, w_branch, w_gate, conv_taps, rate_blocks, input_blocks, decay_param, w_mix, gain_pre, gain_post):
    normed = norm_rows(tokens, gain_pre).astype(jnp.bfloat16)
    branch = jnp.dot(normed, w_branch, preferred_element_type=jnp.float32).astype(jnp.bfloat16)
    gate_act = jnp.dot(normed, w_gate, preferred_element_type=jnp.float32).astype(jnp.bfloat16)
    window = jnp.concatenate([conv_state, branch[:, None, :]], axis=1)
    convolved = lax.optimization_barrier(jnp.sum(window.astype(jnp.float32) * conv_taps.astype(jnp.float32)[None], axis=1))
    row_count, branch_width = convolved.shape
    blocks = rate_blocks.shape[0]
    pieces = convolved.reshape(row_count, blocks, branch_width // blocks)
    rate_gate = jax.nn.sigmoid(jnp.einsum('snc,ncd->snd', pieces, rate_blocks.astype(jnp.float32)).reshape(row_count, branch_width))
    inflow = jax.nn.sigmoid(jnp.einsum('snc,ncd->snd', pieces, input_blocks.astype(jnp.float32)).reshape(row_count, branch_width))
    log_decay = -gate_scale * rate_gate * jax.nn.softplus(-decay_param.astype(jnp.float32))
    state_next = jnp.exp(log_decay) * recur_state + jnp.sqrt(-jnp.expm1(2.0 * log_decay)) * (inflow * convolved)
    merged = (state_next * jax.nn.gelu(gate_act.astype(jnp.float32))).astype(jnp.bfloat16)
    mix_out = jnp.dot(merged, w_mix, preferred_element_type=jnp.float32).astype(jnp.bfloat16)
    residual = tokens.astype(jnp.float32) + norm_rows(mix_out, gain_post)
    return (residual, window[:, 1:, :], state_next)

def expert_rows(bundle):
    row_block, gate_w, up_w, down_w = bundle
    gate_part = jnp.dot(row_block, gate_w, preferred_element_type=jnp.float32)
    up_part = jnp.dot(row_block, up_w, preferred_element_type=jnp.float32)
    hidden = (jax.nn.silu(gate_part) * up_part).astype(jnp.bfloat16)
    return jnp.dot(hidden, down_w, preferred_element_type=jnp.float32).astype(jnp.bfloat16)

def reference(tokens, conv_state, recur_state, w_branch, w_gate, conv_taps, rate_blocks, input_blocks, decay_param, w_mix, gain_pre, gain_post, gain_ffn, gain_out, routes, affinity, w_expert_gate, w_expert_up, w_expert_down):
    residual, conv_next, state_next = recurrence(tokens, conv_state, recur_state, w_branch, w_gate, conv_taps, rate_blocks, input_blocks, decay_param, w_mix, gain_pre, gain_post)
    ffn_in = norm_rows(residual, gain_ffn).astype(jnp.bfloat16)
    flat_routes = routes.reshape(-1).astype(jnp.int32)
    onehot = (flat_routes[:, None] == jnp.arange(EXPERTS, dtype=jnp.int32)[None, :]).astype(jnp.int32)
    rank_all = lax.optimization_barrier(jnp.sum(jnp.cumsum(onehot, axis=0) * onehot, axis=1)) - 1
    kept_rows = rank_all < LIMIT
    target = jnp.where(kept_rows, flat_routes * LIMIT + rank_all, EXPERTS * LIMIT).astype(jnp.int32)
    repeated = jnp.repeat(ffn_in, TOP_K, axis=0)
    buffer = jnp.zeros((EXPERTS * LIMIT + 1, D), jnp.bfloat16).at[target].set(repeated)
    grouped = buffer[:EXPERTS * LIMIT].reshape(EXPERTS, LIMIT, D)
    outputs = lax.map(expert_rows, (grouped, w_expert_gate, w_expert_up, w_expert_down))
    out_table = jnp.concatenate([outputs.reshape(EXPERTS * LIMIT, D), jnp.zeros((1, D), jnp.bfloat16)], axis=0)
    picked = jnp.take(out_table, target, axis=0).astype(jnp.float32).reshape(TOKENS, TOP_K, D)
    weights = affinity / lax.optimization_barrier(jnp.sum(affinity, axis=1, keepdims=True))
    combined = lax.optimization_barrier(jnp.sum(weights[:, :, None] * picked, axis=1))
    layer_out = (residual + norm_rows(combined, gain_out)).astype(jnp.bfloat16)
    return (layer_out, conv_next, state_next)
```

```python
import functools

import jax
import jax.numpy as jnp
from jax import lax
from jax.experimental import pallas as pl
from jax.experimental.pallas import tpu as pltpu
from jax.sharding import PartitionSpec as P

epsilon = 1e-06
gate_scale = 8.0
line = 8
lanes = 128
stride = 3
tile = 256
wide = 512


def rms(values, gain):
    return values * lax.rsqrt(jnp.mean(values * values, axis=-1, keepdims=True) + epsilon) * gain


def layer_kernel(
    n, cap, limit, top,
    tokens, conv_state, recur, taps, rate_b, input_b, decay_param,
    g_pre, g_post, g_ffn, g_out, routes, affinity,
    wb_hbm, wg_hbm, wm_hbm, eg_hbm, eu_hbm, ed_hbm,
    out, conv_out, state_out,
    wb, wg, wm, eg, eu, ed, normed, merged, mix, residual, rate_w, input_w,
    stage, rows_x, packed, sbuf, rbuf, obuf, cbuf, otile,
    mrow, mall, tab_v, share_v, etab_v, tab, share, etab,
    load_sem, tab_sem, m_send, m_recv, s_send, s_recv, o_send, o_recv, ready,
):
    f32, bf16 = jnp.float32, jnp.bfloat16
    me = lax.axis_index("ep")
    rows, width = tokens.shape
    channels = recur.shape[1]
    block = rate_b.shape[1]
    parts = width // lanes
    lots = n // line
    outer, inner = me // line, lax.rem(me, line)

    pairs = []
    for t in range(channels // tile):
        cols = pl.ds(t * tile, tile)
        pairs.append((wb_hbm.at[:, cols], wb.at[:, cols]))
        pairs.append((wg_hbm.at[:, cols], wg.at[:, cols]))
    first_mix = len(pairs)
    for t in range(width // wide):
        cols = pl.ds(t * wide, wide)
        pairs.append((wm_hbm.at[:, cols], wm.at[:, cols]))
    first_expert = len(pairs)
    pairs += [(eg_hbm.at[0], eg), (eu_hbm.at[0], eu), (ed_hbm.at[0], ed)]
    loads = [pltpu.make_async_copy(src, dst, load_sem.at[k]) for k, (src, dst) in enumerate(pairs)]
    for load in loads:
        load.start()

    beside = [outer * line + lax.rem(inner + d, line) for d in range(1, line)]
    along = [lax.rem(outer + q, lots) * line + inner for q in range(1, lots)]
    barrier = pltpu.get_barrier_semaphore()
    for device in along + beside:
        pl.semaphore_signal(barrier, inc=1, device_id={"ep": device})

    def rcopy(src, dst, send, recv, device):
        return pltpu.make_async_remote_copy(
            src_ref=src, dst_ref=dst, send_sem=send, recv_sem=recv,
            device_id={"ep": device}, device_id_type=pl.DeviceIdType.MESH,
        )

    flat = top * rows
    row_at = lax.broadcasted_iota(jnp.int32, (flat, flat), 0)
    col_at = lax.broadcasted_iota(jnp.int32, (flat, flat), 1)
    row_s, col_s = lax.rem(row_at, rows), lax.rem(col_at, rows)
    named = jnp.concatenate([routes[k : k + 1, :] for k in range(top)], axis=1)
    mrow[...] = named
    mall[me] = named
    down = jnp.transpose(jnp.broadcast_to(named, (8, flat)))[:, 0:1]
    equal = down == named
    rank_row = jnp.sum(jnp.where(equal & (row_s < col_s), 1, 0), axis=0, keepdims=True)
    rank_col = jnp.sum(jnp.where(equal & (col_s < row_s), 1, 0), axis=1, keepdims=True)
    mine = down == col_at
    table = [
        jnp.sum(jnp.where(mine & (rank_col == r), row_s, 0), axis=0, keepdims=True)
        for r in range(cap)
    ]
    table.append(named * cap + rank_row)
    table += [jnp.zeros((1, flat), jnp.int32)] * (8 - len(table))
    tab_v[...] = jnp.concatenate(table, axis=0)
    amount = affinity[...]
    part = amount / jnp.sum(amount, axis=0, keepdims=True)
    part = jnp.concatenate([part[k : k + 1, :] for k in range(top)], axis=1)
    share_v[...] = jnp.broadcast_to(part, (8, flat))
    to_tab = pltpu.make_async_copy(tab_v, tab, tab_sem.at[0])
    to_share = pltpu.make_async_copy(share_v, share, tab_sem.at[1])
    to_tab.start()
    to_share.start()

    normed[...] = rms(tokens[...].astype(f32), g_pre[...]).astype(bf16)

    same = lax.broadcasted_iota(jnp.int32, (tile, tile), 0) // block == (
        lax.broadcasted_iota(jnp.int32, (tile, tile), 1) // block
    )
    for ref, spread in ((rate_b, rate_w), (input_b, input_w)):
        for t in range(channels // tile):
            piece = ref[pl.ds(t * tile, tile), :].astype(f32)
            spread[t] = jnp.where(
                same, jnp.concatenate([piece] * (tile // block), axis=1), 0.0
            ).astype(bf16)

    softplus = jnp.maximum(-decay_param[...], 0.0) + jnp.log1p(jnp.exp(-jnp.abs(decay_param[...])))
    slope = -gate_scale * softplus
    conv_out[0] = conv_state[1]
    conv_out[1] = conv_state[2]

    pl.semaphore_wait(barrier, len(along) + len(beside))
    for device in beside:
        pl.semaphore_signal(ready, inc=1, device_id={"ep": device})
    for device in beside:
        rcopy(mrow, mall.at[me], m_send.at[0], m_recv.at[0], device).start()

    for t in range(channels // tile):
        cols = slice(t * tile, (t + 1) * tile)
        loads[2 * t].wait()
        branch = jnp.dot(normed[...], wb[:, cols], preferred_element_type=f32).astype(bf16)
        conv_out[2, :, cols] = branch
        conv = branch.astype(f32) * taps[3:4, cols]
        for k in range(3):
            conv = conv + conv_state[k, :, cols].astype(f32) * taps[k : k + 1, cols]
        conv16 = conv.astype(bf16)
        rate = jax.nn.sigmoid(jnp.dot(conv16, rate_w[t], preferred_element_type=f32))
        inflow = jax.nn.sigmoid(jnp.dot(conv16, input_w[t], preferred_element_type=f32))
        log_decay = rate * slope[:, cols]
        decay = jnp.exp(log_decay)
        rest = -jnp.tanh(log_decay) * (decay * decay + 1.0)
        state = decay * recur[:, cols] + jnp.sqrt(rest) * (inflow * conv)
        state_out[:, cols] = state
        loads[2 * t + 1].wait()
        gate = jnp.dot(normed[...], wg[:, cols], preferred_element_type=f32).astype(bf16)
        merged[:, cols] = (state * jax.nn.gelu(gate.astype(f32))).astype(bf16)

    rcopy(mall.at[pl.ds(0, line - 1)], mall.at[pl.ds(0, line - 1)], m_send.at[0], m_recv.at[0], me).wait_recv()
    ours = pl.ds(outer * line, line)
    for device in along:
        rcopy(mall.at[ours], mall.at[ours], m_send.at[1], m_recv.at[1], device).start()

    for t in range(width // wide):
        cols = slice(t * wide, (t + 1) * wide)
        loads[first_mix + t].wait()
        mix[:, cols] = (
            jnp.dot(merged[...], wm[:, cols], preferred_element_type=f32).astype(bf16).astype(f32)
        )
    residual[...] = tokens[...].astype(f32) + rms(mix[...], g_post[...])
    ffn = rms(residual[...], g_ffn[...])
    for j in range(parts):
        stage[pl.ds(j, rows, stride=parts), :] = ffn[:, j * lanes : (j + 1) * lanes]
    rows_x[...] = stage[...].reshape(rows, parts, lanes).astype(bf16)
    to_tab.wait()
    to_share.wait()

    @pl.loop(0, n, unroll=4)
    def _(e):
        for r in range(cap):
            sbuf[e * cap + r] = rows_x[tab[r, e]]

    def block_of(device):
        return pl.ds(device * cap, cap)

    pl.semaphore_wait(ready, len(beside))

    @pl.loop(1, n)
    def _(i):
        device = lax.rem(me + stride * i, n)
        rcopy(sbuf.at[block_of(device)], rbuf.at[block_of(me)], s_send, s_recv, device).start()

    for r in range(cap):
        rbuf[me * cap + r] = sbuf[me * cap + r]

    rcopy(mall.at[pl.ds(0, n - line)], mall.at[pl.ds(0, n - line)], m_send.at[1], m_recv.at[1], me).wait_recv()
    every = mall[...].reshape(n, flat)
    count = jnp.sum(jnp.where(every == me, 1, 0), axis=1, keepdims=True)
    dev_row = lax.broadcasted_iota(jnp.int32, (n, n), 0)
    dev_col = lax.broadcasted_iota(jnp.int32, (n, n), 1)
    base_row = jnp.sum(jnp.where(dev_row < dev_col, count, 0), axis=0, keepdims=True)
    base_col = jnp.sum(jnp.where(dev_row == dev_col, base_row, 0), axis=1, keepdims=True)
    origin = jnp.sum(
        jnp.where(
            (base_col <= dev_col) & (dev_col < base_col + count),
            dev_row * cap + dev_col - base_col, 0,
        ),
        axis=0, keepdims=True,
    )
    table = [origin] + [jnp.minimum(base_row + r, limit) for r in range(cap)]
    table += [jnp.zeros((1, n), jnp.int32)] * (8 - len(table))
    etab_v[...] = jnp.concatenate(table, axis=0)
    to_etab = pltpu.make_async_copy(etab_v, etab, tab_sem.at[2])
    to_etab.start()
    to_etab.wait()
    for load in loads[first_expert:]:
        load.wait()
    otile[limit] = jnp.zeros((parts, lanes), bf16)

    most = pl.ds(0, (n - 1) * cap)
    rcopy(sbuf.at[most], rbuf.at[most], s_send, s_recv, me).wait_recv()

    @pl.loop(0, limit, unroll=4)
    def _(p):
        stage[pl.ds(pl.multiple_of(p * parts, parts), parts), :] = rbuf[etab[0, p]].astype(f32)

    for j in range(parts):
        packed[:, j * lanes : (j + 1) * lanes] = stage[pl.ds(j, limit, stride=parts), :].astype(bf16)
    x = packed[...]
    gate = jnp.dot(x, eg[...], preferred_element_type=f32)
    up = jnp.dot(x, eu[...], preferred_element_type=f32)
    hidden = (jax.nn.silu(gate) * up).astype(bf16)
    for t in range(width // wide):
        result = jnp.dot(hidden, ed[:, t * wide : (t + 1) * wide], preferred_element_type=f32)
        for j in range(wide // lanes):
            stage[pl.ds(t * (wide // lanes) + j, limit, stride=parts), :] = (
                result[:, j * lanes : (j + 1) * lanes]
            )
    otile[pl.ds(0, limit)] = stage[...].reshape(limit, parts, lanes).astype(bf16)

    @pl.loop(0, n, unroll=4)
    def _(d):
        for r in range(cap):
            obuf[d * cap + r] = otile[etab[1 + r, d]]

    @pl.loop(1, n)
    def _(i):
        device = lax.rem(me + stride * i, n)
        rcopy(obuf.at[block_of(device)], cbuf.at[block_of(me)], o_send, o_recv, device).start()

    for r in range(cap):
        cbuf[me * cap + r] = obuf[me * cap + r]

    rcopy(obuf.at[most], cbuf.at[most], o_send, o_recv, me).wait_recv()

    @pl.loop(0, rows, unroll=4)
    def _(s):
        value = jnp.zeros((parts, lanes), f32)
        for k in range(top):
            value = value + share[0, k * rows + s] * cbuf[tab[cap, k * rows + s]].astype(f32)
        stage[pl.ds(pl.multiple_of(s * parts, parts), parts), :] = value

    squares = jnp.zeros((rows, 1), f32)
    for j in range(parts):
        cols = slice(j * lanes, (j + 1) * lanes)
        piece = stage[pl.ds(j, rows, stride=parts), :]
        mix[:, cols] = piece
        squares = squares + jnp.sum(piece * piece, axis=1, keepdims=True)
    scale = lax.rsqrt(squares / width + epsilon)
    out[...] = (residual[...] + mix[...] * scale * g_out[...]).astype(out.dtype)

    head = pl.ds(0, line - 1)
    rest_of = pl.ds(0, (lots - 1) * line)
    rcopy(mall.at[head], mall.at[head], m_send.at[0], m_recv.at[0], me).wait_send()
    rcopy(mall.at[rest_of], mall.at[rest_of], m_send.at[1], m_recv.at[1], me).wait_send()
    rcopy(sbuf.at[most], rbuf.at[most], s_send, s_recv, me).wait_send()
    rcopy(obuf.at[most], cbuf.at[most], o_send, o_recv, me).wait_send()


def finish_kernel(a, b, c, a_out, b_out, c_out, a_buf, b_buf, c_buf, get, put):
    work = ((a, a_buf, a_out), (b, b_buf, b_out), (c, c_buf, c_out))
    ins = [pltpu.make_async_copy(src, buf, get.at[k]) for k, (src, buf, _) in enumerate(work)]
    outs = [pltpu.make_async_copy(buf, dst, put.at[k]) for k, (_, buf, dst) in enumerate(work)]
    for copy in ins:
        copy.start()
    for load, store in zip(ins, outs):
        load.wait()
        store.start()
    for copy in outs:
        copy.wait()


def vmem(count):
    return [pl.BlockSpec(memory_space=pltpu.VMEM)] * count


def hbm(count):
    return [pl.BlockSpec(memory_space=pltpu.HBM)] * count


def shards(
    tokens, conv_state, recur_state, w_branch, w_gate, conv_taps, rate_blocks, input_blocks,
    decay_param, w_mix, gain_pre, gain_post, gain_ffn, gain_out, routes, affinity,
    w_expert_gate, w_expert_up, w_expert_down,
):
    n = lax.axis_size("ep")
    rows, width = tokens.shape
    channels = recur_state.shape[1]
    top = routes.shape[1]
    hidden = w_expert_gate.shape[2]
    bf16, f32, i32 = jnp.bfloat16, jnp.float32, jnp.int32
    cap, limit = 3, 64
    parts = width // lanes
    row = lambda v: v.reshape(1, -1)
    block = rate_blocks.shape[1]
    dma = pltpu.SemaphoreType.DMA
    shapes = (
        jax.ShapeDtypeStruct((rows, width), bf16),
        jax.ShapeDtypeStruct((3, rows, channels), bf16),
        jax.ShapeDtypeStruct((rows, channels), f32),
    )
    exchange = pltpu.VMEM((n * cap, parts, lanes), bf16)
    results = pl.pallas_call(
        functools.partial(layer_kernel, n, cap, limit, top),
        out_shape=shapes,
        in_specs=vmem(13) + hbm(6),
        out_specs=tuple(vmem(3)),
        scratch_shapes=[
            pltpu.VMEM((width, channels), bf16),
            pltpu.VMEM((width, channels), bf16),
            pltpu.VMEM((channels, width), bf16),
            pltpu.VMEM((width, hidden), bf16),
            pltpu.VMEM((width, hidden), bf16),
            pltpu.VMEM((hidden, width), bf16),
            pltpu.VMEM((rows, width), bf16),
            pltpu.VMEM((rows, channels), bf16),
            pltpu.VMEM((rows, width), f32),
            pltpu.VMEM((rows, width), f32),
            pltpu.VMEM((channels // tile, tile, tile), bf16),
            pltpu.VMEM((channels // tile, tile, tile), bf16),
            pltpu.VMEM((rows * parts, lanes), f32),
            pltpu.VMEM((rows, parts, lanes), bf16),
            pltpu.VMEM((limit, width), bf16),
            exchange, exchange, exchange, exchange,
            pltpu.VMEM((limit + 1, parts, lanes), bf16),
            pltpu.VMEM((1, top * rows), i32),
            pltpu.VMEM((n, 1, top * rows), i32),
            pltpu.VMEM((8, top * rows), i32),
            pltpu.VMEM((8, top * rows), f32),
            pltpu.VMEM((8, n), i32),
            pltpu.SMEM((8, top * rows), i32),
            pltpu.SMEM((8, top * rows), f32),
            pltpu.SMEM((8, n), i32),
            dma((2 * channels // tile + width // wide + 3,)),
            dma((3,)), dma((2,)), dma((2,)), dma, dma, dma, dma,
            pltpu.SemaphoreType.REGULAR,
        ],
        compiler_params=pltpu.CompilerParams(
            collective_id=0, has_side_effects=True, vmem_limit_bytes=60 << 20
        ),
    )(
        tokens, conv_state.transpose(1, 0, 2), recur_state, conv_taps,
        rate_blocks.reshape(channels, block), input_blocks.reshape(channels, block),
        row(decay_param), row(gain_pre), row(gain_post), row(gain_ffn), row(gain_out),
        routes.T, affinity.T,
        w_branch, w_gate, w_mix, w_expert_gate, w_expert_up, w_expert_down,
    )
    layer_out, conv_next, state_next = pl.pallas_call(
        finish_kernel,
        out_shape=shapes,
        in_specs=hbm(3),
        out_specs=tuple(hbm(3)),
        scratch_shapes=[pltpu.VMEM(s.shape, s.dtype) for s in shapes] + [dma((3,)), dma((3,))],
    )(*results)
    return (layer_out, conv_next.transpose(1, 0, 2), state_next)


def solution(mesh):
    ep, copied = "ep", P()
    return jax.shard_map(
        shards,
        mesh=mesh,
        in_specs=(P(ep, None), P(ep, None, None), P(ep, None))
        + (copied,) * 11
        + (P(ep, None),) * 2
        + (P(ep, None, None),) * 3,
        out_specs=(P(ep, None), P(ep, None, None), P(ep, None)),
        check_vma=False,
    )
```

```python
import functools

import jax
import jax.numpy as jnp
from jax import lax
from jax.experimental import pallas as pl
from jax.experimental.pallas import tpu as pltpu
from jax.sharding import PartitionSpec as P

epsilon = 1e-06
gate_scale = 8.0
line = 8
lanes = 128
stride = 3
ahead = 4
tile = 256
wide = 512


def rms(values, gain):
    return values * lax.rsqrt(jnp.mean(values * values, axis=-1, keepdims=True) + epsilon) * gain


def layer_kernel(
    n, cap, limit, top,
    tokens_hbm, conv_hbm, recur_hbm, taps_hbm, rate_hbm, input_hbm, decay_hbm,
    pre_hbm, post_hbm, ffn_hbm, last_hbm, routes_hbm, affinity_hbm,
    wb_hbm, wg_hbm, wm_hbm, eg_hbm, eu_hbm, ed_hbm,
    out_hbm, conv_out_hbm, state_out_hbm,
    tokens, conv_state, recur, taps, rate_b, input_b, decay_param,
    g_pre, g_post, g_ffn, g_out, routes, affinity,
    out, conv_out, state_out,
    wb, wg, wm, eg, eu, ed, normed, branch_b, gate_b, merged, mix, residual, rate_w, input_w,
    stage, rows_x, packed, sbuf, rbuf_a, rbuf_b, obuf, cbuf, otile,
    mrow, mall, tab_v, share_v, etab_v, tab, share, etab,
    load_sem, small_sem, put_sem, tab_sem, m_send, m_recv, s_send, s_recv, o_send, o_recv,
):
    f32, bf16 = jnp.float32, jnp.bfloat16
    me = lax.axis_index("ep")
    rows, width = tokens.shape
    channels = recur.shape[1]
    block = rate_b.shape[1]
    parts = width // lanes
    lots = n // line
    half = n // 2
    turn = pow(stride, -1, n)

    pairs = []
    for t in range(channels // tile):
        cols = pl.ds(t * tile, tile)
        pairs.append((wb_hbm.at[:, cols], wb.at[:, cols]))
        pairs.append((wg_hbm.at[:, cols], wg.at[:, cols]))
    first_mix = len(pairs)
    for t in range(width // wide):
        cols = pl.ds(t * wide, wide)
        pairs.append((wm_hbm.at[:, cols], wm.at[:, cols]))
    first_expert = len(pairs)
    pairs += [(eg_hbm.at[0], eg), (eu_hbm.at[0], eu), (ed_hbm.at[0], ed)]
    loads = [pltpu.make_async_copy(src, dst, load_sem.at[k]) for k, (src, dst) in enumerate(pairs)]
    smalls = [
        pltpu.make_async_copy(src, dst, small_sem.at[k])
        for k, (src, dst) in enumerate(
            (
                (routes_hbm, routes), (affinity_hbm, affinity), (tokens_hbm, tokens),
                (pre_hbm, g_pre), (rate_hbm, rate_b), (input_hbm, input_b), (decay_hbm, decay_param),
                (conv_hbm, conv_state), (taps_hbm, taps), (recur_hbm, recur),
                (post_hbm, g_post), (ffn_hbm, g_ffn), (last_hbm, g_out),
            )
        )
    ]
    for load in smalls + loads[:4]:
        load.start()

    barrier = pltpu.get_barrier_semaphore()

    def greet(i):
        pl.semaphore_signal(barrier, inc=1, device_id={"ep": lax.rem(me + i, n)})

    def each_peer(step):
        @pl.loop(0, lots - 1)
        def _(k):
            for j in range(line):
                step(k * line + j + 1)

        for i in range((lots - 1) * line + 1, n):
            step(i)

    each_peer(greet)
    for load in loads[4:first_mix]:
        load.start()

    def rcopy(src, dst, send, recv, device):
        return pltpu.make_async_remote_copy(
            src_ref=src, dst_ref=dst, send_sem=send, recv_sem=recv,
            device_id={"ep": device}, device_id_type=pl.DeviceIdType.MESH,
        )

    for load in smalls[:2]:
        load.wait()
    flat = top * rows
    row_at = lax.broadcasted_iota(jnp.int32, (flat, flat), 0)
    col_at = lax.broadcasted_iota(jnp.int32, (flat, flat), 1)
    row_s, col_s = lax.rem(row_at, rows), lax.rem(col_at, rows)
    named = jnp.concatenate([routes[k : k + 1, :] for k in range(top)], axis=1)
    mrow[...] = named
    mall[me] = named
    across = lax.rem((named - me + n) * turn, n)
    down = jnp.transpose(jnp.broadcast_to(across, (8, flat)))[:, 0:1]
    equal = down == across
    rank_row = jnp.sum(jnp.where(equal & (row_s < col_s), 1, 0), axis=0, keepdims=True)
    rank_col = jnp.sum(jnp.where(equal & (col_s < row_s), 1, 0), axis=1, keepdims=True)
    mine = down == col_at
    table = [
        jnp.sum(jnp.where(mine & (rank_col == r), row_s, 0), axis=0, keepdims=True)
        for r in range(cap)
    ]
    table.append(across * cap + jnp.minimum(rank_row, cap - 1))
    table += [jnp.zeros((1, flat), jnp.int32)] * (8 - len(table))
    tab_v[...] = jnp.concatenate(table, axis=0)
    amount = affinity[...]
    part = amount / jnp.sum(amount, axis=0, keepdims=True)
    part = jnp.concatenate([part[k : k + 1, :] for k in range(top)], axis=1)
    share_v[...] = jnp.broadcast_to(part, (8, flat))
    to_tab = pltpu.make_async_copy(tab_v, tab, tab_sem.at[0])
    to_share = pltpu.make_async_copy(share_v, share, tab_sem.at[1])
    to_tab.start()
    to_share.start()

    for load in smalls[2:4]:
        load.wait()
    normed[...] = rms(tokens[...].astype(f32), g_pre[...]).astype(bf16)

    for load in loads[first_mix:first_expert]:
        load.start()
    for load in smalls[4:]:
        load.wait()
    same = lax.broadcasted_iota(jnp.int32, (tile, tile), 0) // block == (
        lax.broadcasted_iota(jnp.int32, (tile, tile), 1) // block
    )
    for ref, spread in ((rate_b, rate_w), (input_b, input_w)):
        for t in range(channels // tile):
            piece = ref[pl.ds(t * tile, tile), :].astype(f32)
            spread[t] = jnp.where(
                same, jnp.concatenate([piece] * (tile // block), axis=1), 0.0
            ).astype(bf16)

    softplus = jnp.maximum(-decay_param[...], 0.0) + jnp.log1p(jnp.exp(-jnp.abs(decay_param[...])))
    slope = -gate_scale * softplus
    conv_out[0] = conv_state[1]
    conv_out[1] = conv_state[2]

    steps = channels // tile
    for t in range(steps + 1):
        if t < steps:
            cols = slice(t * tile, (t + 1) * tile)
            loads[2 * t].wait()
            loads[2 * t + 1].wait()
            branch_b[:, cols] = jnp.dot(
                normed[...], wb[:, cols], preferred_element_type=f32
            ).astype(bf16)
            gate_b[:, cols] = jnp.dot(
                normed[...], wg[:, cols], preferred_element_type=f32
            ).astype(bf16)
        if t > 0:
            cols = slice((t - 1) * tile, t * tile)
            branch = branch_b[:, cols]
            conv_out[2, :, cols] = branch
            conv = branch.astype(f32) * taps[3:4, cols]
            for k in range(3):
                conv = conv + conv_state[k, :, cols].astype(f32) * taps[k : k + 1, cols]
            conv16 = conv.astype(bf16)
            rate = jax.nn.sigmoid(jnp.dot(conv16, rate_w[t - 1], preferred_element_type=f32))
            inflow = jax.nn.sigmoid(jnp.dot(conv16, input_w[t - 1], preferred_element_type=f32))
            log_decay = rate * slope[:, cols]
            decay = jnp.exp(log_decay)
            rest = -jnp.tanh(log_decay) * (decay * decay + 1.0)
            state = decay * recur[:, cols] + jnp.sqrt(rest) * (inflow * conv)
            state_out[:, cols] = state
            merged[:, cols] = (state * jax.nn.gelu(gate_b[:, cols].astype(f32))).astype(bf16)

    pl.semaphore_wait(barrier, n - 1)

    def tell(i):
        rcopy(mrow, mall.at[me], m_send, m_recv, lax.rem(me + stride * i, n)).start()

    each_peer(tell)

    for t in range(width // wide):
        cols = slice(t * wide, (t + 1) * wide)
        loads[first_mix + t].wait()
        mix[:, cols] = (
            jnp.dot(merged[...], wm[:, cols], preferred_element_type=f32).astype(bf16).astype(f32)
        )
    for load in loads[first_expert:]:
        load.start()
    residual[...] = tokens[...].astype(f32) + rms(mix[...], g_post[...])
    ffn = rms(residual[...], g_ffn[...])
    for j in range(parts):
        stage[pl.ds(j, rows, stride=parts), :] = ffn[:, j * lanes : (j + 1) * lanes]
    rows_x[...] = stage[...].reshape(rows, parts, lanes).astype(bf16)
    to_tab.wait()
    to_share.wait()

    def block_of(i):
        return pl.ds(i * cap, cap)

    def fetch(i):
        for r in range(cap):
            sbuf[i * cap + r] = rows_x[tab[r, i]]

    def send(i, landing, origin, k):
        rcopy(
            sbuf.at[block_of(i)], landing.at[block_of(i - origin)], s_send.at[k], s_recv.at[k],
            lax.rem(me + stride * i, n),
        ).start()

    for i in range(ahead + 1):
        fetch(i)

    @pl.loop(1, half)
    def _(i):
        fetch(i + ahead)
        send(i, rbuf_a, 0, 0)

    @pl.loop(half, n - ahead)
    def _(i):
        fetch(i + ahead)
        send(i, rbuf_b, half, 1)

    for i in range(n - ahead, n):
        send(i, rbuf_b, half, 1)

    put_conv = pltpu.make_async_copy(conv_out, conv_out_hbm, put_sem.at[0])
    put_state = pltpu.make_async_copy(state_out, state_out_hbm, put_sem.at[1])
    put_conv.start()
    put_state.start()
    rbuf_a[block_of(0)] = sbuf[block_of(0)]

    others = pl.ds(0, n - 1)
    rcopy(mall.at[others], mall.at[others], m_send, m_recv, me).wait_recv()
    every = mall[...].reshape(n, flat)
    count = jnp.minimum(jnp.sum(jnp.where(every == me, 1, 0), axis=1, keepdims=True), cap)
    dev_row = lax.broadcasted_iota(jnp.int32, (n, n), 0)
    dev_col = lax.broadcasted_iota(jnp.int32, (n, n), 1)
    eye = dev_row == dev_col
    earlier = dev_row < dev_col

    def turned(column):
        return jnp.sum(jnp.where(eye, column, 0), axis=0, keepdims=True)

    def upright(line_of):
        return jnp.sum(jnp.where(eye, line_of, 0), axis=1, keepdims=True)

    def before(column):
        return jnp.sum(jnp.where(earlier, column, 0), axis=0, keepdims=True)

    kept = jnp.clip(limit - upright(before(count)), 0, count)
    slot = lax.rem((me - dev_row[:, 0:1] + n) * turn, n)
    soon = slot < half
    place = jnp.where(
        lax.rem((me - dev_col[0:1, :] + n) * turn, n) < half,
        before(jnp.where(soon, kept, 0)), before(jnp.where(soon, 0, kept)),
    )
    place_col = upright(place)
    inside = (place_col <= dev_col) & (dev_col < place_col + kept)
    origin = slot * cap + dev_col - place_col
    table = [
        jnp.sum(jnp.where(inside & soon, origin, 0), axis=0, keepdims=True),
        jnp.sum(jnp.where(inside & (slot >= half), origin - half * cap, 0), axis=0, keepdims=True),
    ]
    kept_row = turned(kept)
    table += [jnp.where(kept_row > r, place + r, limit) for r in range(cap)]
    table += [jnp.zeros((1, n), jnp.int32)] * (8 - len(table))
    etab_v[...] = jnp.concatenate(table, axis=0)
    to_etab = pltpu.make_async_copy(etab_v, etab, tab_sem.at[2])
    to_etab.start()
    to_etab.wait()
    for load in loads[first_expert:]:
        load.wait()
    otile[limit] = jnp.zeros((parts, lanes), bf16)

    def fetch_back(i):
        device = lax.rem(me - stride * i + stride * n, n)
        for r in range(cap):
            obuf[i * cap + r] = otile[etab[2 + r, device]]

    def send_back(i, k):
        rcopy(
            obuf.at[block_of(i)], cbuf.at[block_of(i)], o_send.at[k], o_recv.at[k],
            lax.rem(me - stride * i + stride * n, n),
        ).start()

    def expert(landing, k):
        @pl.loop(0, limit, unroll=4)
        def _(p):
            stage[pl.ds(pl.multiple_of(p * parts, parts), parts), :] = (
                landing[etab[k, p]].astype(f32)
            )

        for j in range(parts):
            packed[:, j * lanes : (j + 1) * lanes] = (
                stage[pl.ds(j, limit, stride=parts), :].astype(bf16)
            )
        x = packed[...]
        gate = jnp.dot(x, eg[...], preferred_element_type=f32)
        up = jnp.dot(x, eu[...], preferred_element_type=f32)
        hidden = (jax.nn.silu(gate) * up).astype(bf16)
        for t in range(width // wide):
            result = jnp.dot(hidden, ed[:, t * wide : (t + 1) * wide], preferred_element_type=f32)
            for j in range(wide // lanes):
                stage[pl.ds(t * (wide // lanes) + j, limit, stride=parts), :] = (
                    result[:, j * lanes : (j + 1) * lanes]
                )
        otile[pl.ds(0, limit)] = stage[...].reshape(limit, parts, lanes).astype(bf16)

    def wait_rows(landing, count_of, k):
        some = pl.ds(0, count_of * cap)
        rcopy(sbuf.at[some], landing.at[some], s_send.at[k], s_recv.at[k], me).wait_recv()

    wait_rows(rbuf_a, half - 1, 0)
    expert(rbuf_a, 0)
    for i in range(ahead + 1):
        fetch_back(i)

    @pl.loop(1, half - ahead)
    def _(i):
        fetch_back(i + ahead)
        send_back(i, 0)

    for i in range(half - ahead, half):
        send_back(i, 0)
    cbuf[block_of(0)] = obuf[block_of(0)]

    wait_rows(rbuf_b, n - half, 1)
    expert(rbuf_b, 1)
    for i in range(half, half + ahead):
        fetch_back(i)

    @pl.loop(half, n - ahead)
    def _(i):
        fetch_back(i + ahead)
        send_back(i, 1)

    for i in range(n - ahead, n):
        send_back(i, 1)

    low, high = pl.ds(0, (half - 1) * cap), pl.ds(0, (n - half) * cap)
    rcopy(obuf.at[low], cbuf.at[low], o_send.at[0], o_recv.at[0], me).wait_recv()
    rcopy(obuf.at[high], cbuf.at[high], o_send.at[1], o_recv.at[1], me).wait_recv()

    @pl.loop(0, rows, unroll=4)
    def _(s):
        value = jnp.zeros((parts, lanes), f32)
        for k in range(top):
            value = value + share[0, k * rows + s] * cbuf[tab[cap, k * rows + s]].astype(f32)
        stage[pl.ds(pl.multiple_of(s * parts, parts), parts), :] = value

    squares = jnp.zeros((rows, 1), f32)
    for j in range(parts):
        cols = slice(j * lanes, (j + 1) * lanes)
        piece = stage[pl.ds(j, rows, stride=parts), :]
        mix[:, cols] = piece
        squares = squares + jnp.sum(piece * piece, axis=1, keepdims=True)
    scale = lax.rsqrt(squares / width + epsilon)
    out[...] = (residual[...] + mix[...] * scale * g_out[...]).astype(out.dtype)
    put_out = pltpu.make_async_copy(out, out_hbm, put_sem.at[2])
    put_out.start()

    rcopy(mall.at[others], mall.at[others], m_send, m_recv, me).wait_send()
    for k, some in enumerate((low, high)):
        rcopy(sbuf.at[some], cbuf.at[some], s_send.at[k], s_recv.at[k], me).wait_send()
        rcopy(obuf.at[some], cbuf.at[some], o_send.at[k], o_recv.at[k], me).wait_send()
    put_conv.wait()
    put_state.wait()
    put_out.wait()


def finish_kernel(a, b, c, a_out, b_out, c_out, a_buf, b_buf, c_buf, get, put):
    work = ((a, a_buf, a_out), (b, b_buf, b_out), (c, c_buf, c_out))
    ins = [pltpu.make_async_copy(src, buf, get.at[k]) for k, (src, buf, _) in enumerate(work)]
    outs = [pltpu.make_async_copy(buf, dst, put.at[k]) for k, (_, buf, dst) in enumerate(work)]
    for copy in ins:
        copy.start()
    for load, store in zip(ins, outs):
        load.wait()
        store.start()
    for copy in outs:
        copy.wait()


def hbm(count):
    return [pl.BlockSpec(memory_space=pltpu.HBM)] * count


def shards(
    tokens, conv_state, recur_state, w_branch, w_gate, conv_taps, rate_blocks, input_blocks,
    decay_param, w_mix, gain_pre, gain_post, gain_ffn, gain_out, routes, affinity,
    w_expert_gate, w_expert_up, w_expert_down,
):
    n = lax.axis_size("ep")
    rows, width = tokens.shape
    channels = recur_state.shape[1]
    top = routes.shape[1]
    hidden = w_expert_gate.shape[2]
    bf16, f32, i32 = jnp.bfloat16, jnp.float32, jnp.int32
    cap, limit = 3, 64
    parts = width // lanes
    row = lambda v: v.reshape(1, -1)
    block = rate_blocks.shape[1]
    dma = pltpu.SemaphoreType.DMA
    shapes = (
        jax.ShapeDtypeStruct((rows, width), bf16),
        jax.ShapeDtypeStruct((3, rows, channels), bf16),
        jax.ShapeDtypeStruct((rows, channels), f32),
    )
    small = (
        tokens, conv_state.transpose(1, 0, 2), recur_state, conv_taps,
        rate_blocks.reshape(channels, block), input_blocks.reshape(channels, block),
        row(decay_param), row(gain_pre), row(gain_post), row(gain_ffn), row(gain_out),
        routes.T, affinity.T,
    )
    half = n // 2
    exchange = pltpu.VMEM((n * cap, parts, lanes), bf16)
    exchange_a = pltpu.VMEM((half * cap, parts, lanes), bf16)
    exchange_b = pltpu.VMEM(((n - half) * cap, parts, lanes), bf16)
    results = pl.pallas_call(
        functools.partial(layer_kernel, n, cap, limit, top),
        out_shape=shapes,
        in_specs=hbm(19),
        out_specs=tuple(hbm(3)),
        scratch_shapes=[pltpu.VMEM(v.shape, v.dtype) for v in small + shapes]
        + [
            pltpu.VMEM((width, channels), bf16),
            pltpu.VMEM((width, channels), bf16),
            pltpu.VMEM((channels, width), bf16),
            pltpu.VMEM((width, hidden), bf16),
            pltpu.VMEM((width, hidden), bf16),
            pltpu.VMEM((hidden, width), bf16),
            pltpu.VMEM((rows, width), bf16),
            pltpu.VMEM((rows, channels), bf16),
            pltpu.VMEM((rows, channels), bf16),
            pltpu.VMEM((rows, channels), bf16),
            pltpu.VMEM((rows, width), f32),
            pltpu.VMEM((rows, width), f32),
            pltpu.VMEM((channels // tile, tile, tile), bf16),
            pltpu.VMEM((channels // tile, tile, tile), bf16),
            pltpu.VMEM((rows * parts, lanes), f32),
            pltpu.VMEM((rows, parts, lanes), bf16),
            pltpu.VMEM((limit, width), bf16),
            exchange, exchange_a, exchange_b, exchange, exchange,
            pltpu.VMEM((limit + 1, parts, lanes), bf16),
            pltpu.VMEM((1, top * rows), i32),
            pltpu.VMEM((n, 1, top * rows), i32),
            pltpu.VMEM((8, top * rows), i32),
            pltpu.VMEM((8, top * rows), f32),
            pltpu.VMEM((8, n), i32),
            pltpu.SMEM((8, top * rows), i32),
            pltpu.SMEM((8, top * rows), f32),
            pltpu.SMEM((8, n), i32),
            dma((2 * channels // tile + width // wide + 3,)),
            dma((len(small),)), dma((3,)), dma((3,)), dma, dma, dma((2,)), dma((2,)), dma((2,)), dma((2,)),
        ],
        compiler_params=pltpu.CompilerParams(
            collective_id=0, has_side_effects=True, vmem_limit_bytes=60 << 20
        ),
    )(
        *small, w_branch, w_gate, w_mix, w_expert_gate, w_expert_up, w_expert_down,
    )
    layer_out, conv_next, state_next = pl.pallas_call(
        finish_kernel,
        out_shape=shapes,
        in_specs=hbm(3),
        out_specs=tuple(hbm(3)),
        scratch_shapes=[pltpu.VMEM(s.shape, s.dtype) for s in shapes] + [dma((3,)), dma((3,))],
    )(*results)
    return (layer_out, conv_next.transpose(1, 0, 2), state_next)


def solution(mesh):
    ep, copied = "ep", P()
    return jax.shard_map(
        shards,
        mesh=mesh,
        in_specs=(P(ep, None), P(ep, None, None), P(ep, None))
        + (copied,) * 11
        + (P(ep, None),) * 2
        + (P(ep, None, None),) * 3,
        out_specs=(P(ep, None), P(ep, None, None), P(ep, None)),
        check_vma=False,
    )
```

```python
import functools

import jax
import jax.numpy as jnp
from jax import lax
from jax.experimental import pallas as pl
from jax.experimental.pallas import tpu as pltpu
from jax.sharding import PartitionSpec as P

epsilon = 1e-06
gate_scale = 8.0
line = 8
lanes = 128
stride = 21
ahead = 4
tile = 256
wide = 512


def rms(values, gain):
    return values * lax.rsqrt(jnp.mean(values * values, axis=-1, keepdims=True) + epsilon) * gain


def layer_kernel(
    n, cap, limit, top,
    tokens_hbm, conv_hbm, recur_hbm, taps_hbm, rate_hbm, input_hbm, decay_hbm,
    pre_hbm, post_hbm, ffn_hbm, last_hbm, routes_hbm, affinity_hbm,
    wb_hbm, wg_hbm, wm_hbm, eg_hbm, eu_hbm, ed_hbm,
    out_hbm, conv_out_hbm, state_out_hbm,
    tokens, conv_state, recur, taps, rate_b, input_b, decay_param,
    g_pre, g_post, g_ffn, g_out, routes, affinity,
    out, conv_out, state_out,
    wb, wg, wm, eg, eu, ed, normed, branch_b, gate_b, merged, mix, residual, rate_w, input_w,
    stage, rows_x, packed, sbuf, rbuf_a, rbuf_b, obuf, cbuf, otile,
    mrow, mall, tab_v, share_v, etab_v, tab, share, etab,
    load_sem, small_sem, put_sem, tab_sem, m_send, m_recv, s_send, s_recv, o_send, o_recv,
):
    f32, bf16 = jnp.float32, jnp.bfloat16
    me = lax.axis_index("ep")
    rows, width = tokens.shape
    channels = recur.shape[1]
    block = rate_b.shape[1]
    parts = width // lanes
    lots = n // line
    half = n // 2
    turn = pow(stride, -1, n)

    pairs = []
    for t in range(channels // tile):
        cols = pl.ds(t * tile, tile)
        pairs.append((wb_hbm.at[:, cols], wb.at[:, cols]))
        pairs.append((wg_hbm.at[:, cols], wg.at[:, cols]))
    first_mix = len(pairs)
    for t in range(width // wide):
        cols = pl.ds(t * wide, wide)
        pairs.append((wm_hbm.at[:, cols], wm.at[:, cols]))
    first_expert = len(pairs)
    pairs += [(eg_hbm.at[0], eg), (eu_hbm.at[0], eu), (ed_hbm.at[0], ed)]
    loads = [pltpu.make_async_copy(src, dst, load_sem.at[k]) for k, (src, dst) in enumerate(pairs)]
    smalls = [
        pltpu.make_async_copy(src, dst, small_sem.at[k])
        for k, (src, dst) in enumerate(
            (
                (routes_hbm, routes), (affinity_hbm, affinity), (tokens_hbm, tokens),
                (pre_hbm, g_pre), (rate_hbm, rate_b), (input_hbm, input_b), (decay_hbm, decay_param),
                (conv_hbm, conv_state), (taps_hbm, taps), (recur_hbm, recur),
                (post_hbm, g_post), (ffn_hbm, g_ffn), (last_hbm, g_out),
            )
        )
    ]
    for load in smalls[:4] + loads[:2]:
        load.start()

    barrier = pltpu.get_barrier_semaphore()

    def greet(i):
        pl.semaphore_signal(barrier, inc=1, device_id={"ep": lax.rem(me + i, n)})

    def peers(step, begin, end):
        count = (end - begin) // line

        @pl.loop(0, count)
        def _(k):
            for j in range(line):
                step(begin + k * line + j)

        for i in range(begin + count * line, end):
            step(i)

    peers(greet, 1, n // 2)
    for load in smalls[4:] + loads[2:4]:
        load.start()
    peers(greet, n // 2, n)
    for load in loads[4:first_mix]:
        load.start()

    def rcopy(src, dst, send, recv, device):
        return pltpu.make_async_remote_copy(
            src_ref=src, dst_ref=dst, send_sem=send, recv_sem=recv,
            device_id={"ep": device}, device_id_type=pl.DeviceIdType.MESH,
        )

    for load in smalls[:2]:
        load.wait()
    flat = top * rows
    row_at = lax.broadcasted_iota(jnp.int32, (flat, flat), 0)
    col_at = lax.broadcasted_iota(jnp.int32, (flat, flat), 1)
    row_s, col_s = lax.rem(row_at, rows), lax.rem(col_at, rows)
    named = jnp.concatenate([routes[k : k + 1, :] for k in range(top)], axis=1)
    mrow[...] = named
    mall[me] = named
    across = lax.rem((named - me + n) * turn, n)
    down = jnp.transpose(jnp.broadcast_to(across, (8, flat)))[:, 0:1]
    equal = down == across
    rank_row = jnp.sum(jnp.where(equal & (row_s < col_s), 1, 0), axis=0, keepdims=True)
    rank_col = jnp.sum(jnp.where(equal & (col_s < row_s), 1, 0), axis=1, keepdims=True)
    mine = down == col_at
    table = [
        jnp.sum(jnp.where(mine & (rank_col == r), row_s, 0), axis=0, keepdims=True)
        for r in range(cap)
    ]
    table.append(across * cap + jnp.minimum(rank_row, cap - 1))
    table += [jnp.zeros((1, flat), jnp.int32)] * (8 - len(table))
    tab_v[...] = jnp.concatenate(table, axis=0)
    amount = affinity[...]
    part = amount / jnp.sum(amount, axis=0, keepdims=True)
    part = jnp.concatenate([part[k : k + 1, :] for k in range(top)], axis=1)
    share_v[...] = jnp.broadcast_to(part, (8, flat))
    to_tab = pltpu.make_async_copy(tab_v, tab, tab_sem.at[0])
    to_share = pltpu.make_async_copy(share_v, share, tab_sem.at[1])
    to_tab.start()
    to_share.start()

    for load in smalls[2:4]:
        load.wait()
    normed[...] = rms(tokens[...].astype(f32), g_pre[...]).astype(bf16)

    for load in loads[first_mix:first_expert]:
        load.start()
    steps = channels // tile
    for t in range(steps + 1):
        if t < steps:
            cols = slice(t * tile, (t + 1) * tile)
            loads[2 * t].wait()
            loads[2 * t + 1].wait()
            if t == 1:
                for load in smalls[4:]:
                    load.wait()
            branch_b[:, cols] = jnp.dot(
                normed[...], wb[:, cols], preferred_element_type=f32
            ).astype(bf16)
            gate_b[:, cols] = jnp.dot(
                normed[...], wg[:, cols], preferred_element_type=f32
            ).astype(bf16)
        if t == 1:
            same = lax.broadcasted_iota(jnp.int32, (tile, tile), 0) // block == (
                lax.broadcasted_iota(jnp.int32, (tile, tile), 1) // block
            )
            for ref, spread in ((rate_b, rate_w), (input_b, input_w)):
                for u in range(steps):
                    piece = ref[pl.ds(u * tile, tile), :].astype(f32)
                    spread[u] = jnp.where(
                        same, jnp.concatenate([piece] * (tile // block), axis=1), 0.0
                    ).astype(bf16)

            softplus = jnp.maximum(-decay_param[...], 0.0) + jnp.log1p(jnp.exp(-jnp.abs(decay_param[...])))
            slope = -gate_scale * softplus
            conv_out[0] = conv_state[1]
            conv_out[1] = conv_state[2]

        if t > 0:
            cols = slice((t - 1) * tile, t * tile)
            branch = branch_b[:, cols]
            conv_out[2, :, cols] = branch
            conv = branch.astype(f32) * taps[3:4, cols]
            for k in range(3):
                conv = conv + conv_state[k, :, cols].astype(f32) * taps[k : k + 1, cols]
            conv16 = conv.astype(bf16)
            rate = jax.nn.sigmoid(jnp.dot(conv16, rate_w[t - 1], preferred_element_type=f32))
            inflow = jax.nn.sigmoid(jnp.dot(conv16, input_w[t - 1], preferred_element_type=f32))
            log_decay = rate * slope[:, cols]
            decay = jnp.exp(log_decay)
            rest = -jnp.tanh(log_decay) * (decay * decay + 1.0)
            state = decay * recur[:, cols] + jnp.sqrt(rest) * (inflow * conv)
            state_out[:, cols] = state
            merged[:, cols] = (state * jax.nn.gelu(gate_b[:, cols].astype(f32))).astype(bf16)

    pl.semaphore_wait(barrier, n - 1)

    def tell(i):
        rcopy(mrow, mall.at[me], m_send, m_recv, lax.rem(me + stride * i, n)).start()

    peers(tell, 1, n)

    for load in loads[first_mix:first_expert]:
        load.wait()
    for t in range(width // wide):
        cols = slice(t * wide, (t + 1) * wide)
        mix[:, cols] = (
            jnp.dot(merged[...], wm[:, cols], preferred_element_type=f32).astype(bf16).astype(f32)
        )
    for load in loads[first_expert:]:
        load.start()
    residual[...] = tokens[...].astype(f32) + rms(mix[...], g_post[...])
    ffn = rms(residual[...], g_ffn[...])
    for j in range(parts):
        stage[pl.ds(j, rows, stride=parts), :] = ffn[:, j * lanes : (j + 1) * lanes]
    rows_x[...] = stage[...].reshape(rows, parts, lanes).astype(bf16)
    to_tab.wait()
    to_share.wait()

    def block_of(i):
        return pl.ds(i * cap, cap)

    def fetch(i):
        for r in range(cap):
            sbuf[i * cap + r] = rows_x[tab[r, i]]

    def send(i, landing, origin, k):
        rcopy(
            sbuf.at[block_of(i)], landing.at[block_of(i - origin)], s_send.at[k], s_recv.at[k],
            lax.rem(me + stride * i, n),
        ).start()

    for i in range(ahead + 1):
        fetch(i)

    @pl.loop(1, half)
    def _(i):
        fetch(i + ahead)
        send(i, rbuf_a, 0, 0)

    @pl.loop(half, n - ahead)
    def _(i):
        fetch(i + ahead)
        send(i, rbuf_b, half, 1)

    for i in range(n - ahead, n):
        send(i, rbuf_b, half, 1)

    put_conv = pltpu.make_async_copy(conv_out, conv_out_hbm, put_sem.at[0])
    put_state = pltpu.make_async_copy(state_out, state_out_hbm, put_sem.at[1])
    put_conv.start()
    put_state.start()
    rbuf_a[block_of(0)] = sbuf[block_of(0)]

    others = pl.ds(0, n - 1)
    rcopy(mall.at[others], mall.at[others], m_send, m_recv, me).wait_recv()
    every = mall[...].reshape(n, flat)
    count = jnp.minimum(jnp.sum(jnp.where(every == me, 1, 0), axis=1, keepdims=True), cap)
    dev_row = lax.broadcasted_iota(jnp.int32, (n, n), 0)
    dev_col = lax.broadcasted_iota(jnp.int32, (n, n), 1)
    eye = dev_row == dev_col
    earlier = dev_row < dev_col

    def turned(column):
        return jnp.sum(jnp.where(eye, column, 0), axis=0, keepdims=True)

    def upright(line_of):
        return jnp.sum(jnp.where(eye, line_of, 0), axis=1, keepdims=True)

    def before(column):
        return jnp.sum(jnp.where(earlier, column, 0), axis=0, keepdims=True)

    kept = jnp.clip(limit - upright(before(count)), 0, count)
    slot = lax.rem((me - dev_row[:, 0:1] + n) * turn, n)
    soon = slot < half
    place = jnp.where(
        lax.rem((me - dev_col[0:1, :] + n) * turn, n) < half,
        before(jnp.where(soon, kept, 0)), before(jnp.where(soon, 0, kept)),
    )
    place_col = upright(place)
    inside = (place_col <= dev_col) & (dev_col < place_col + kept)
    origin = slot * cap + dev_col - place_col
    table = [
        jnp.sum(jnp.where(inside & soon, origin, 0), axis=0, keepdims=True),
        jnp.sum(jnp.where(inside & (slot >= half), origin - half * cap, 0), axis=0, keepdims=True),
    ]
    kept_row = turned(kept)
    table += [jnp.where(kept_row > r, place + r, limit) for r in range(cap)]
    table += [jnp.zeros((1, n), jnp.int32)] * (8 - len(table))
    etab_v[...] = jnp.concatenate(table, axis=0)
    to_etab = pltpu.make_async_copy(etab_v, etab, tab_sem.at[2])
    to_etab.start()
    to_etab.wait()
    for load in loads[first_expert:]:
        load.wait()
    otile[limit] = jnp.zeros((parts, lanes), bf16)

    def fetch_back(i):
        device = lax.rem(me - stride * i + stride * n, n)
        for r in range(cap):
            obuf[i * cap + r] = otile[etab[2 + r, device]]

    def send_back(i, k):
        rcopy(
            obuf.at[block_of(i)], cbuf.at[block_of(i)], o_send.at[k], o_recv.at[k],
            lax.rem(me - stride * i + stride * n, n),
        ).start()

    def expert(landing, k):
        @pl.loop(0, limit, unroll=4)
        def _(p):
            stage[pl.ds(pl.multiple_of(p * parts, parts), parts), :] = (
                landing[etab[k, p]].astype(f32)
            )

        for j in range(parts):
            packed[:, j * lanes : (j + 1) * lanes] = (
                stage[pl.ds(j, limit, stride=parts), :].astype(bf16)
            )
        x = packed[...]
        gate = jnp.dot(x, eg[...], preferred_element_type=f32)
        up = jnp.dot(x, eu[...], preferred_element_type=f32)
        hidden = (jax.nn.silu(gate) * up).astype(bf16)
        for t in range(width // wide):
            result = jnp.dot(hidden, ed[:, t * wide : (t + 1) * wide], preferred_element_type=f32)
            for j in range(wide // lanes):
                stage[pl.ds(t * (wide // lanes) + j, limit, stride=parts), :] = (
                    result[:, j * lanes : (j + 1) * lanes]
                )
        otile[pl.ds(0, limit)] = stage[...].reshape(limit, parts, lanes).astype(bf16)

    def wait_rows(landing, count_of, k):
        some = pl.ds(0, count_of * cap)
        rcopy(sbuf.at[some], landing.at[some], s_send.at[k], s_recv.at[k], me).wait_recv()

    wait_rows(rbuf_a, half - 1, 0)
    expert(rbuf_a, 0)
    for i in range(ahead + 1):
        fetch_back(i)

    @pl.loop(1, half - ahead)
    def _(i):
        fetch_back(i + ahead)
        send_back(i, 0)

    for i in range(half - ahead, half):
        send_back(i, 0)
    cbuf[block_of(0)] = obuf[block_of(0)]

    wait_rows(rbuf_b, n - half, 1)
    expert(rbuf_b, 1)
    for i in range(half, half + ahead):
        fetch_back(i)

    @pl.loop(half, n - ahead)
    def _(i):
        fetch_back(i + ahead)
        send_back(i, 1)

    for i in range(n - ahead, n):
        send_back(i, 1)

    low, high = pl.ds(0, (half - 1) * cap), pl.ds(0, (n - half) * cap)
    rcopy(obuf.at[low], cbuf.at[low], o_send.at[0], o_recv.at[0], me).wait_recv()
    rcopy(obuf.at[high], cbuf.at[high], o_send.at[1], o_recv.at[1], me).wait_recv()

    @pl.loop(0, rows, unroll=4)
    def _(s):
        value = jnp.zeros((parts, lanes), f32)
        for k in range(top):
            value = value + share[0, k * rows + s] * cbuf[tab[cap, k * rows + s]].astype(f32)
        stage[pl.ds(pl.multiple_of(s * parts, parts), parts), :] = value

    squares = jnp.zeros((rows, 1), f32)
    for j in range(parts):
        cols = slice(j * lanes, (j + 1) * lanes)
        piece = stage[pl.ds(j, rows, stride=parts), :]
        mix[:, cols] = piece
        squares = squares + jnp.sum(piece * piece, axis=1, keepdims=True)
    scale = lax.rsqrt(squares / width + epsilon)
    out[...] = (residual[...] + mix[...] * scale * g_out[...]).astype(out.dtype)
    put_out = pltpu.make_async_copy(out, out_hbm, put_sem.at[2])
    put_out.start()

    rcopy(mall.at[others], mall.at[others], m_send, m_recv, me).wait_send()
    for k, some in enumerate((low, high)):
        rcopy(sbuf.at[some], cbuf.at[some], s_send.at[k], s_recv.at[k], me).wait_send()
        rcopy(obuf.at[some], cbuf.at[some], o_send.at[k], o_recv.at[k], me).wait_send()
    put_conv.wait()
    put_state.wait()
    put_out.wait()


def finish_kernel(a, b, c, a_out, b_out, c_out, a_buf, b_buf, c_buf, get, put):
    work = ((a, a_buf, a_out), (b, b_buf, b_out), (c, c_buf, c_out))
    ins = [pltpu.make_async_copy(src, buf, get.at[k]) for k, (src, buf, _) in enumerate(work)]
    outs = [pltpu.make_async_copy(buf, dst, put.at[k]) for k, (_, buf, dst) in enumerate(work)]
    for copy in ins:
        copy.start()
    for load, store in zip(ins, outs):
        load.wait()
        store.start()
    for copy in outs:
        copy.wait()


def hbm(count):
    return [pl.BlockSpec(memory_space=pltpu.HBM)] * count


def shards(
    tokens, conv_state, recur_state, w_branch, w_gate, conv_taps, rate_blocks, input_blocks,
    decay_param, w_mix, gain_pre, gain_post, gain_ffn, gain_out, routes, affinity,
    w_expert_gate, w_expert_up, w_expert_down,
):
    n = lax.axis_size("ep")
    rows, width = tokens.shape
    channels = recur_state.shape[1]
    top = routes.shape[1]
    hidden = w_expert_gate.shape[2]
    bf16, f32, i32 = jnp.bfloat16, jnp.float32, jnp.int32
    cap, limit = 3, 64
    parts = width // lanes
    row = lambda v: v.reshape(1, -1)
    block = rate_blocks.shape[1]
    dma = pltpu.SemaphoreType.DMA
    shapes = (
        jax.ShapeDtypeStruct((rows, width), bf16),
        jax.ShapeDtypeStruct((3, rows, channels), bf16),
        jax.ShapeDtypeStruct((rows, channels), f32),
    )
    small = (
        tokens, conv_state.transpose(1, 0, 2), recur_state, conv_taps,
        rate_blocks.reshape(channels, block), input_blocks.reshape(channels, block),
        row(decay_param), row(gain_pre), row(gain_post), row(gain_ffn), row(gain_out),
        routes.T, affinity.T,
    )
    half = n // 2
    exchange = pltpu.VMEM((n * cap, parts, lanes), bf16)
    exchange_a = pltpu.VMEM((half * cap, parts, lanes), bf16)
    exchange_b = pltpu.VMEM(((n - half) * cap, parts, lanes), bf16)
    results = pl.pallas_call(
        functools.partial(layer_kernel, n, cap, limit, top),
        out_shape=shapes,
        in_specs=hbm(19),
        out_specs=tuple(hbm(3)),
        scratch_shapes=[pltpu.VMEM(v.shape, v.dtype) for v in small + shapes]
        + [
            pltpu.VMEM((width, channels), bf16),
            pltpu.VMEM((width, channels), bf16),
            pltpu.VMEM((channels, width), bf16),
            pltpu.VMEM((width, hidden), bf16),
            pltpu.VMEM((width, hidden), bf16),
            pltpu.VMEM((hidden, width), bf16),
            pltpu.VMEM((rows, width), bf16),
            pltpu.VMEM((rows, channels), bf16),
            pltpu.VMEM((rows, channels), bf16),
            pltpu.VMEM((rows, channels), bf16),
            pltpu.VMEM((rows, width), f32),
            pltpu.VMEM((rows, width), f32),
            pltpu.VMEM((channels // tile, tile, tile), bf16),
            pltpu.VMEM((channels // tile, tile, tile), bf16),
            pltpu.VMEM((rows * parts, lanes), f32),
            pltpu.VMEM((rows, parts, lanes), bf16),
            pltpu.VMEM((limit, width), bf16),
            exchange, exchange_a, exchange_b, exchange, exchange,
            pltpu.VMEM((limit + 1, parts, lanes), bf16),
            pltpu.VMEM((1, top * rows), i32),
            pltpu.VMEM((n, 1, top * rows), i32),
            pltpu.VMEM((8, top * rows), i32),
            pltpu.VMEM((8, top * rows), f32),
            pltpu.VMEM((8, n), i32),
            pltpu.SMEM((8, top * rows), i32),
            pltpu.SMEM((8, top * rows), f32),
            pltpu.SMEM((8, n), i32),
            dma((2 * channels // tile + width // wide + 3,)),
            dma((len(small),)), dma((3,)), dma((3,)), dma, dma, dma((2,)), dma((2,)), dma((2,)), dma((2,)),
        ],
        compiler_params=pltpu.CompilerParams(
            collective_id=0, has_side_effects=True, vmem_limit_bytes=60 << 20
        ),
    )(
        *small, w_branch, w_gate, w_mix, w_expert_gate, w_expert_up, w_expert_down,
    )
    layer_out, conv_next, state_next = pl.pallas_call(
        finish_kernel,
        out_shape=shapes,
        in_specs=hbm(3),
        out_specs=tuple(hbm(3)),
        scratch_shapes=[pltpu.VMEM(s.shape, s.dtype) for s in shapes] + [dma((3,)), dma((3,))],
    )(*results)
    return (layer_out, conv_next.transpose(1, 0, 2), state_next)


def solution(mesh):
    ep, copied = "ep", P()
    return jax.shard_map(
        shards,
        mesh=mesh,
        in_specs=(P(ep, None), P(ep, None, None), P(ep, None))
        + (copied,) * 11
        + (P(ep, None),) * 2
        + (P(ep, None, None),) * 3,
        out_specs=(P(ep, None), P(ep, None, None), P(ep, None)),
        check_vma=False,
    )
```

```python
import functools

import jax
import jax.numpy as jnp
from jax import lax
from jax.experimental import pallas as pl
from jax.experimental.pallas import tpu as pltpu
from jax.sharding import PartitionSpec as P

epsilon = 1e-06
gate_scale = 8.0
line = 8
lanes = 128
stride = 21
ahead = 4
tile = 256
wide = 512


def rms(values, gain):
    return values * lax.rsqrt(jnp.mean(values * values, axis=-1, keepdims=True) + epsilon) * gain


def layer_kernel(
    n, cap, limit, top,
    tokens_hbm, conv_hbm, recur_hbm, taps_hbm, rate_hbm, input_hbm, decay_hbm,
    pre_hbm, post_hbm, ffn_hbm, last_hbm, routes_hbm, affinity_hbm,
    wb_hbm, wg_hbm, wm_hbm, eg_hbm, eu_hbm, ed_hbm,
    out_hbm, conv_out_hbm, state_out_hbm,
    tokens, conv_state, recur, taps, rate_b, input_b, decay_param,
    g_pre, g_post, g_ffn, g_out, routes, affinity,
    out, conv_out, state_out,
    wb, wg, wm, eg, eu, ed, normed, branch_b, gate_b, merged, mix, residual, rate_w, input_w,
    stage, rows_x, packed, sbuf, rbuf_a, rbuf_b, obuf, cbuf, otile,
    mrow, mall, tab_v, share_v, etab_v, tab, share, etab,
    load_sem, small_sem, put_sem, tab_sem, m_send, m_recv, s_send, s_recv, o_send, o_recv,
):
    f32, bf16 = jnp.float32, jnp.bfloat16
    me = lax.axis_index("ep")
    rows, width = tokens.shape
    channels = recur.shape[1]
    block = rate_b.shape[1]
    parts = width // lanes
    lots = n // line
    half = n // 2
    turn = pow(stride, -1, n)

    pairs = []
    for t in range(channels // tile):
        cols = pl.ds(t * tile, tile)
        pairs.append((wb_hbm.at[:, cols], wb.at[:, cols]))
        pairs.append((wg_hbm.at[:, cols], wg.at[:, cols]))
    first_mix = len(pairs)
    for t in range(width // wide):
        cols = pl.ds(t * wide, wide)
        pairs.append((wm_hbm.at[:, cols], wm.at[:, cols]))
    first_expert = len(pairs)
    pairs += [(eg_hbm.at[0], eg), (eu_hbm.at[0], eu), (ed_hbm.at[0], ed)]
    loads = [pltpu.make_async_copy(src, dst, load_sem.at[k]) for k, (src, dst) in enumerate(pairs)]
    smalls = [
        pltpu.make_async_copy(src, dst, small_sem.at[k])
        for k, (src, dst) in enumerate(
            (
                (routes_hbm, routes), (affinity_hbm, affinity), (tokens_hbm, tokens),
                (pre_hbm, g_pre), (rate_hbm, rate_b), (input_hbm, input_b), (decay_hbm, decay_param),
                (conv_hbm, conv_state), (taps_hbm, taps), (recur_hbm, recur),
                (post_hbm, g_post), (ffn_hbm, g_ffn), (last_hbm, g_out),
            )
        )
    ]
    for load in smalls[:4] + loads[:2]:
        load.start()

    barrier = pltpu.get_barrier_semaphore()

    def greet(i):
        pl.semaphore_signal(barrier, inc=1, device_id={"ep": lax.rem(me + i, n)})

    def peers(step, begin, end):
        count = (end - begin) // line

        @pl.loop(0, count)
        def _(k):
            for j in range(line):
                step(begin + k * line + j)

        for i in range(begin + count * line, end):
            step(i)

    peers(greet, 1, n // 2)
    for load in smalls[4:] + loads[2:4]:
        load.start()
    peers(greet, n // 2, n)
    for load in loads[4:first_mix]:
        load.start()

    def rcopy(src, dst, send, recv, device):
        return pltpu.make_async_remote_copy(
            src_ref=src, dst_ref=dst, send_sem=send, recv_sem=recv,
            device_id={"ep": device}, device_id_type=pl.DeviceIdType.MESH,
        )

    for load in smalls[:2]:
        load.wait()
    flat = top * rows
    row_at = lax.broadcasted_iota(jnp.int32, (flat, flat), 0)
    col_at = lax.broadcasted_iota(jnp.int32, (flat, flat), 1)
    row_s, col_s = lax.rem(row_at, rows), lax.rem(col_at, rows)
    named = jnp.concatenate([routes[k : k + 1, :] for k in range(top)], axis=1)
    mrow[...] = named
    mall[me] = named
    across = lax.rem((named - me + n) * turn, n)
    down = jnp.transpose(jnp.broadcast_to(across, (8, flat)))[:, 0:1]
    equal = down == across
    rank_row = jnp.sum(jnp.where(equal & (row_s < col_s), 1, 0), axis=0, keepdims=True)
    rank_col = jnp.sum(jnp.where(equal & (col_s < row_s), 1, 0), axis=1, keepdims=True)
    mine = down == col_at
    table = [
        jnp.sum(jnp.where(mine & (rank_col == r), row_s, 0), axis=0, keepdims=True)
        for r in range(cap)
    ]
    table.append(across * cap + jnp.minimum(rank_row, cap - 1))
    table += [jnp.zeros((1, flat), jnp.int32)] * (8 - len(table))
    tab_v[...] = jnp.concatenate(table, axis=0)
    amount = affinity[...]
    part = amount / jnp.sum(amount, axis=0, keepdims=True)
    part = jnp.concatenate([part[k : k + 1, :] for k in range(top)], axis=1)
    share_v[...] = jnp.broadcast_to(part, (8, flat))
    to_tab = pltpu.make_async_copy(tab_v, tab, tab_sem.at[0])
    to_share = pltpu.make_async_copy(share_v, share, tab_sem.at[1])
    to_tab.start()
    to_share.start()

    for load in smalls[2:4]:
        load.wait()
    normed[...] = rms(tokens[...].astype(f32), g_pre[...]).astype(bf16)

    for load in loads[first_mix:first_expert]:
        load.start()
    steps = channels // tile
    for t in range(steps + 1):
        if t < steps:
            cols = slice(t * tile, (t + 1) * tile)
            loads[2 * t].wait()
            loads[2 * t + 1].wait()
            if t == 1:
                for load in smalls[4:]:
                    load.wait()
            branch_b[:, cols] = jnp.dot(
                normed[...], wb[:, cols], preferred_element_type=f32
            ).astype(bf16)
            gate_b[:, cols] = jnp.dot(
                normed[...], wg[:, cols], preferred_element_type=f32
            ).astype(bf16)
        if t == 1:
            same = lax.broadcasted_iota(jnp.int32, (tile, tile), 0) // block == (
                lax.broadcasted_iota(jnp.int32, (tile, tile), 1) // block
            )
            for ref, spread in ((rate_b, rate_w), (input_b, input_w)):
                for u in range(steps):
                    piece = ref[pl.ds(u * tile, tile), :].astype(f32)
                    spread[u] = jnp.where(
                        same, jnp.concatenate([piece] * (tile // block), axis=1), 0.0
                    ).astype(bf16)

            softplus = jnp.maximum(-decay_param[...], 0.0) + jnp.log1p(jnp.exp(-jnp.abs(decay_param[...])))
            slope = -gate_scale * softplus
            conv_out[0] = conv_state[1]
            conv_out[1] = conv_state[2]

        if t > 0:
            cols = slice((t - 1) * tile, t * tile)
            branch = branch_b[:, cols]
            conv_out[2, :, cols] = branch
            conv = branch.astype(f32) * taps[3:4, cols]
            for k in range(3):
                conv = conv + conv_state[k, :, cols].astype(f32) * taps[k : k + 1, cols]
            conv16 = conv.astype(bf16)
            rate = jax.nn.sigmoid(jnp.dot(conv16, rate_w[t - 1], preferred_element_type=f32))
            inflow = jax.nn.sigmoid(jnp.dot(conv16, input_w[t - 1], preferred_element_type=f32))
            log_decay = rate * slope[:, cols]
            decay = jnp.exp(log_decay)
            rest = -jnp.tanh(log_decay) * (decay * decay + 1.0)
            state = decay * recur[:, cols] + jnp.sqrt(rest) * (inflow * conv)
            state_out[:, cols] = state
            merged[:, cols] = (state * jax.nn.gelu(gate_b[:, cols].astype(f32))).astype(bf16)

    pl.semaphore_wait(barrier, n - 1)

    def tell(i):
        rcopy(mrow, mall.at[me], m_send, m_recv, lax.rem(me + stride * i, n)).start()

    peers(tell, 1, n)

    for load in loads[first_mix:first_expert]:
        load.wait()
    for t in range(width // wide):
        cols = slice(t * wide, (t + 1) * wide)
        mix[:, cols] = (
            jnp.dot(merged[...], wm[:, cols], preferred_element_type=f32).astype(bf16).astype(f32)
        )
    for load in loads[first_expert:]:
        load.start()
    residual[...] = tokens[...].astype(f32) + rms(mix[...], g_post[...])
    ffn = rms(residual[...], g_ffn[...])
    for j in range(parts):
        stage[pl.ds(j, rows, stride=parts), :] = ffn[:, j * lanes : (j + 1) * lanes]
    rows_x[...] = stage[...].reshape(rows, parts, lanes).astype(bf16)
    to_tab.wait()
    to_share.wait()

    def block_of(i):
        return pl.ds(i * cap, cap)

    def fetch(i):
        for r in range(cap):
            sbuf[i * cap + r] = rows_x[tab[r, i]]

    def send(i, landing, origin, k):
        rcopy(
            sbuf.at[block_of(i)], landing.at[block_of(i - origin)], s_send.at[k], s_recv.at[k],
            lax.rem(me + stride * i, n),
        ).start()

    for i in range(ahead + 1):
        fetch(i)

    @pl.loop(1, half)
    def _(i):
        fetch(i + ahead)
        send(i, rbuf_a, 0, 0)

    @pl.loop(half, n - ahead)
    def _(i):
        fetch(i + ahead)
        send(i, rbuf_b, half, 1)

    for i in range(n - ahead, n):
        send(i, rbuf_b, half, 1)

    put_conv = pltpu.make_async_copy(conv_out, conv_out_hbm, put_sem.at[0])
    put_state = pltpu.make_async_copy(state_out, state_out_hbm, put_sem.at[1])
    put_conv.start()
    put_state.start()
    rbuf_a[block_of(0)] = sbuf[block_of(0)]

    others = pl.ds(0, n - 1)
    rcopy(mall.at[others], mall.at[others], m_send, m_recv, me).wait_recv()
    every = mall[...].reshape(n, flat)
    count = jnp.minimum(jnp.sum(jnp.where(every == me, 1, 0), axis=1, keepdims=True), cap)
    dev_row = lax.broadcasted_iota(jnp.int32, (n, n), 0)
    dev_col = lax.broadcasted_iota(jnp.int32, (n, n), 1)
    eye = dev_row == dev_col
    earlier = dev_row < dev_col

    def turned(column):
        return jnp.sum(jnp.where(eye, column, 0), axis=0, keepdims=True)

    def upright(line_of):
        return jnp.sum(jnp.where(eye, line_of, 0), axis=1, keepdims=True)

    def before(column):
        return jnp.sum(jnp.where(earlier, column, 0), axis=0, keepdims=True)

    kept = jnp.clip(limit - upright(before(count)), 0, count)
    slot = lax.rem((me - dev_row[:, 0:1] + n) * turn, n)
    soon = slot < half
    place = jnp.where(
        lax.rem((me - dev_col[0:1, :] + n) * turn, n) < half,
        before(jnp.where(soon, kept, 0)), before(jnp.where(soon, 0, kept)),
    )
    place_col = upright(place)
    inside = (place_col <= dev_col) & (dev_col < place_col + kept)
    origin = slot * cap + dev_col - place_col
    table = [
        jnp.sum(jnp.where(inside & soon, origin, 0), axis=0, keepdims=True),
        jnp.sum(jnp.where(inside & (slot >= half), origin - half * cap, 0), axis=0, keepdims=True),
    ]
    kept_row = turned(kept)
    table += [jnp.where(kept_row > r, place + r, limit) for r in range(cap)]
    table += [jnp.zeros((1, n), jnp.int32)] * (8 - len(table))
    etab_v[...] = jnp.concatenate(table, axis=0)
    to_etab = pltpu.make_async_copy(etab_v, etab, tab_sem.at[2])
    to_etab.start()
    to_etab.wait()
    for load in loads[first_expert:]:
        load.wait()
    otile[limit] = jnp.zeros((parts, lanes), bf16)

    def fetch_back(i):
        device = lax.rem(me - stride * i + stride * n, n)
        for r in range(cap):
            obuf[i * cap + r] = otile[etab[2 + r, device]]

    def send_back(i, k):
        rcopy(
            obuf.at[block_of(i)], cbuf.at[block_of(i)], o_send.at[k], o_recv.at[k],
            lax.rem(me - stride * i + stride * n, n),
        ).start()

    def expert(landing, k):
        @pl.loop(0, limit, unroll=8)
        def _(p):
            stage[pl.ds(pl.multiple_of(p * parts, parts), parts), :] = (
                landing[etab[k, p]].astype(f32)
            )

        for j in range(parts):
            packed[:, j * lanes : (j + 1) * lanes] = (
                stage[pl.ds(j, limit, stride=parts), :].astype(bf16)
            )
        x = packed[...]
        gate = jnp.dot(x, eg[...], preferred_element_type=f32)
        up = jnp.dot(x, eu[...], preferred_element_type=f32)
        hidden = (jax.nn.silu(gate) * up).astype(bf16)
        for t in range(width // wide):
            result = jnp.dot(hidden, ed[:, t * wide : (t + 1) * wide], preferred_element_type=f32)
            for j in range(wide // lanes):
                stage[pl.ds(t * (wide // lanes) + j, limit, stride=parts), :] = (
                    result[:, j * lanes : (j + 1) * lanes]
                )
        otile[pl.ds(0, limit)] = stage[...].reshape(limit, parts, lanes).astype(bf16)

    def wait_rows(landing, count_of, k):
        some = pl.ds(0, count_of * cap)
        rcopy(sbuf.at[some], landing.at[some], s_send.at[k], s_recv.at[k], me).wait_recv()

    wait_rows(rbuf_a, half - 1, 0)
    expert(rbuf_a, 0)
    for i in range(ahead + 1):
        fetch_back(i)

    @pl.loop(1, half - ahead)
    def _(i):
        fetch_back(i + ahead)
        send_back(i, 0)

    for i in range(half - ahead, half):
        send_back(i, 0)
    cbuf[block_of(0)] = obuf[block_of(0)]

    wait_rows(rbuf_b, n - half, 1)
    expert(rbuf_b, 1)
    for i in range(half, half + ahead):
        fetch_back(i)

    @pl.loop(half, n - ahead)
    def _(i):
        fetch_back(i + ahead)
        send_back(i, 1)

    for i in range(n - ahead, n):
        send_back(i, 1)

    low, high = pl.ds(0, (half - 1) * cap), pl.ds(0, (n - half) * cap)
    rcopy(obuf.at[low], cbuf.at[low], o_send.at[0], o_recv.at[0], me).wait_recv()
    rcopy(obuf.at[high], cbuf.at[high], o_send.at[1], o_recv.at[1], me).wait_recv()

    @pl.loop(0, rows, unroll=8)
    def _(s):
        value = jnp.zeros((parts, lanes), f32)
        for k in range(top):
            value = value + share[0, k * rows + s] * cbuf[tab[cap, k * rows + s]].astype(f32)
        stage[pl.ds(pl.multiple_of(s * parts, parts), parts), :] = value

    squares = jnp.zeros((rows, 1), f32)
    for j in range(parts):
        cols = slice(j * lanes, (j + 1) * lanes)
        piece = stage[pl.ds(j, rows, stride=parts), :]
        mix[:, cols] = piece
        squares = squares + jnp.sum(piece * piece, axis=1, keepdims=True)
    scale = lax.rsqrt(squares / width + epsilon)
    out[...] = (residual[...] + mix[...] * scale * g_out[...]).astype(out.dtype)
    put_out = pltpu.make_async_copy(out, out_hbm, put_sem.at[2])
    put_out.start()

    rcopy(mall.at[others], mall.at[others], m_send, m_recv, me).wait_send()
    for k, some in enumerate((low, high)):
        rcopy(sbuf.at[some], cbuf.at[some], s_send.at[k], s_recv.at[k], me).wait_send()
        rcopy(obuf.at[some], cbuf.at[some], o_send.at[k], o_recv.at[k], me).wait_send()
    put_conv.wait()
    put_state.wait()
    put_out.wait()


def finish_kernel(a, b, c, a_out, b_out, c_out, a_buf, b_buf, c_buf, get, put):
    work = ((a, a_buf, a_out), (b, b_buf, b_out), (c, c_buf, c_out))
    ins = [pltpu.make_async_copy(src, buf, get.at[k]) for k, (src, buf, _) in enumerate(work)]
    outs = [pltpu.make_async_copy(buf, dst, put.at[k]) for k, (_, buf, dst) in enumerate(work)]
    for copy in ins:
        copy.start()
    for load, store in zip(ins, outs):
        load.wait()
        store.start()
    for copy in outs:
        copy.wait()


def hbm(count):
    return [pl.BlockSpec(memory_space=pltpu.HBM)] * count


def shards(
    tokens, conv_state, recur_state, w_branch, w_gate, conv_taps, rate_blocks, input_blocks,
    decay_param, w_mix, gain_pre, gain_post, gain_ffn, gain_out, routes, affinity,
    w_expert_gate, w_expert_up, w_expert_down,
):
    n = lax.axis_size("ep")
    rows, width = tokens.shape
    channels = recur_state.shape[1]
    top = routes.shape[1]
    hidden = w_expert_gate.shape[2]
    bf16, f32, i32 = jnp.bfloat16, jnp.float32, jnp.int32
    cap, limit = 3, 64
    parts = width // lanes
    row = lambda v: v.reshape(1, -1)
    block = rate_blocks.shape[1]
    dma = pltpu.SemaphoreType.DMA
    shapes = (
        jax.ShapeDtypeStruct((rows, width), bf16),
        jax.ShapeDtypeStruct((3, rows, channels), bf16),
        jax.ShapeDtypeStruct((rows, channels), f32),
    )
    small = (
        tokens, conv_state.transpose(1, 0, 2), recur_state, conv_taps,
        rate_blocks.reshape(channels, block), input_blocks.reshape(channels, block),
        row(decay_param), row(gain_pre), row(gain_post), row(gain_ffn), row(gain_out),
        routes.T, affinity.T,
    )
    half = n // 2
    exchange = pltpu.VMEM((n * cap, parts, lanes), bf16)
    exchange_a = pltpu.VMEM((half * cap, parts, lanes), bf16)
    exchange_b = pltpu.VMEM(((n - half) * cap, parts, lanes), bf16)
    results = pl.pallas_call(
        functools.partial(layer_kernel, n, cap, limit, top),
        out_shape=shapes,
        in_specs=hbm(19),
        out_specs=tuple(hbm(3)),
        scratch_shapes=[pltpu.VMEM(v.shape, v.dtype) for v in small + shapes]
        + [
            pltpu.VMEM((width, channels), bf16),
            pltpu.VMEM((width, channels), bf16),
            pltpu.VMEM((channels, width), bf16),
            pltpu.VMEM((width, hidden), bf16),
            pltpu.VMEM((width, hidden), bf16),
            pltpu.VMEM((hidden, width), bf16),
            pltpu.VMEM((rows, width), bf16),
            pltpu.VMEM((rows, channels), bf16),
            pltpu.VMEM((rows, channels), bf16),
            pltpu.VMEM((rows, channels), bf16),
            pltpu.VMEM((rows, width), f32),
            pltpu.VMEM((rows, width), f32),
            pltpu.VMEM((channels // tile, tile, tile), bf16),
            pltpu.VMEM((channels // tile, tile, tile), bf16),
            pltpu.VMEM((rows * parts, lanes), f32),
            pltpu.VMEM((rows, parts, lanes), bf16),
            pltpu.VMEM((limit, width), bf16),
            exchange, exchange_a, exchange_b, exchange, exchange,
            pltpu.VMEM((limit + 1, parts, lanes), bf16),
            pltpu.VMEM((1, top * rows), i32),
            pltpu.VMEM((n, 1, top * rows), i32),
            pltpu.VMEM((8, top * rows), i32),
            pltpu.VMEM((8, top * rows), f32),
            pltpu.VMEM((8, n), i32),
            pltpu.SMEM((8, top * rows), i32),
            pltpu.SMEM((8, top * rows), f32),
            pltpu.SMEM((8, n), i32),
            dma((2 * channels // tile + width // wide + 3,)),
            dma((len(small),)), dma((3,)), dma((3,)), dma, dma, dma((2,)), dma((2,)), dma((2,)), dma((2,)),
        ],
        compiler_params=pltpu.CompilerParams(
            collective_id=0, has_side_effects=True, vmem_limit_bytes=60 << 20
        ),
    )(
        *small, w_branch, w_gate, w_mix, w_expert_gate, w_expert_up, w_expert_down,
    )
    layer_out, conv_next, state_next = pl.pallas_call(
        finish_kernel,
        out_shape=shapes,
        in_specs=hbm(3),
        out_specs=tuple(hbm(3)),
        scratch_shapes=[pltpu.VMEM(s.shape, s.dtype) for s in shapes] + [dma((3,)), dma((3,))],
    )(*results)
    return (layer_out, conv_next.transpose(1, 0, 2), state_next)


def solution(mesh):
    ep, copied = "ep", P()
    return jax.shard_map(
        shards,
        mesh=mesh,
        in_specs=(P(ep, None), P(ep, None, None), P(ep, None))
        + (copied,) * 11
        + (P(ep, None),) * 2
        + (P(ep, None, None),) * 3,
        out_specs=(P(ep, None), P(ep, None, None), P(ep, None)),
        check_vma=False,
    )
```
